512 devices in a mesh: sp: 16 (over z), fs: 4 (over y), tp: 8 (over x, core).
Axes of the slice: x: 4, y: 4, z: 16, core: 2. Of those that a mesh axis runs over, the one named last changes fastest.
Arguments:
- tokens: bfloat16 [4, 4096, 2048], P('fs', 'sp'), may hold values from -6 to 6
- mix_gain: float32 [2048], replicated, may hold values from 0.1 to 1.9
- query_down: bfloat16 [2048, 768], P('fs', 'tp'), may hold values from -0.125 to 0.125
- memory_down: bfloat16 [2048, 512], P('fs', 'tp'), may hold values from -0.125 to 0.125
- rope_weight: bfloat16 [2048, 32], replicated, may hold values from -0.125 to 0.125
- query_up: bfloat16 [768, 1536], P('fs', 'tp'), may hold values from -0.21875 to 0.21875
- key_up: bfloat16 [512, 1024], P('fs', 'tp'), may hold values from -0.25 to 0.25
- value_up: bfloat16 [512, 1024], P('fs', 'tp'), may hold values from -0.25 to 0.25
- latent_gain: float32 [768], replicated, may hold values from 0.1 to 1.9
- memory_gain: float32 [512], replicated, may hold values from 0.1 to 1.9
- query_gain: float32 [96], replicated, may hold values from 1 to 16
- key_gain: float32 [96], replicated, may hold values from 0.1 to 1.9
- conv_value: bfloat16 [2048, 1024], P('fs', 'tp'), may hold values from -1 to 1
- conv_gate: bfloat16 [2048, 1024], P('fs', 'tp'), may hold values from -0.125 to 0.125
- conv_kernel: bfloat16 [31, 1024], P(None, 'tp'), may hold values from -50 to 50
- channel_gain: float32 [1024], P('tp'), may hold values from 0.1 to 1.9
- channel_shift: float32 [1024], P('tp'), may hold values from -3 to 3
- heads_out: bfloat16 [1024, 2048], P('tp', 'fs'), may hold values from -0.75 to 0.75
- conv_out: bfloat16 [1024, 2048], P('tp', 'fs'), may hold values from -0.1875 to 0.1875
Outputs:
- mixed: bfloat16 [4, 4096, 2048], P('fs', 'sp')
The draws below stay inside these ranges and needn't reach their ends.
All inputs are finite; a program needn't handle non-finite values.
Results may differ from the reference program's by a relative error of at most 0.015.
The reference program's roundings to bfloat16 on the way count: a program that leaves them out, or rounds other values in their place, can miss the bound.
Values may be sent and summed in bfloat16 or wider, within the bound.
A program may use at most 64 MiB of HBM per device.

```python
import math
import jax
import jax.numpy as jnp
from jax import lax

D = 2048
HEADS = 16
QK_NOPE = 64
QK_ROPE = 32
V_DIM = 64
Q_LAT = 768
KV_LAT = 512
CONV_W = 1024
CONV_K = 31
SEG = 64
TOK_DEV = 256
QK_DIM = 96
SEQ = 4096
SEQS = 4
N_TP = 8


def draw_query_gain(key, part):
    gain_key = jax.random.fold_in(key, 11)
    return jnp.exp(jax.random.uniform(gain_key, (QK_DIM,), jnp.float32, 0.0, math.log(3.0)))


def draw_conv_value(key, part):
    noise_key, common_key, level_key = jax.random.split(jax.random.fold_in(key, 23), 3)
    noise = jnp.clip(jax.random.normal(noise_key, (D, CONV_W), jnp.float32), -5.0, 5.0)
    common = jnp.clip(jax.random.normal(common_key, (D,), jnp.float32), -5.0, 5.0)
    level = jax.random.uniform(level_key, (CONV_W,), jnp.float32, 0.5, 1.5)
    strength = 0.7
    return ((noise + strength * common[:, None] * level[None, :]) / math.sqrt(D)).astype(jnp.bfloat16)


def draw_conv_kernel(key, part):
    noise_key, scale_key = jax.random.split(jax.random.fold_in(key, 7))
    channel_pos = jnp.arange(CONV_W, dtype=jnp.float32) / CONV_W
    roughness = jnp.exp(jax.random.uniform(scale_key, (CONV_W,), jnp.float32, -0.7, 0.7))
    channel_scale = 10.0 ** channel_pos * roughness
    tap_draw = jnp.clip(jax.random.normal(noise_key, (CONV_K, CONV_W), jnp.float32), -5.0, 5.0)
    return ((tap_draw + 1.0) * channel_scale[None, :] / math.sqrt(CONV_K)).astype(jnp.bfloat16)


def steps_of(own_key, shape, cuts, least, top_value):
    level, own = 1.0, jax.random.fold_in(own_key, 6)
    for axis_at, shards_of in cuts:
        heights = jnp.exp(jax.random.uniform(jax.random.fold_in(own, axis_at), (shards_of,), jnp.float32, least / len(cuts), top_value / len(cuts)))
        level = level * jnp.repeat(heights, shape[axis_at] // shards_of).reshape([-1 if axis == axis_at else 1 for axis in range(len(shape))])
    return level


def gaussian(own_key, extent, width, reach, cuts=(), kind=jnp.bfloat16):
    factor_of = steps_of(own_key, extent, cuts, -0.22, 0.18) if cuts else 1.0
    drawn = jax.random.normal(own_key, extent, jnp.float32) * width * factor_of
    return jnp.minimum(jnp.maximum(drawn, -reach), reach).astype(kind)


def setup_inputs(seed: int = 0) -> dict:
    arg_keys = jax.random.split(jax.random.key(seed), 20)
    return {
        "tokens": gaussian(arg_keys[0], (SEQS, SEQ, D), 1.0, 6.0, ((0, 4), (1, 16))),
        "mix_gain": jnp.clip(1.0 + 0.18 * jax.random.normal(arg_keys[1], (D,), jnp.float32), 0.1, 1.9),
        "query_down": gaussian(arg_keys[2], (D, Q_LAT), D ** -0.5, 0.125, ((0, 4), (1, 8))),
        "memory_down": gaussian(arg_keys[3], (D, KV_LAT), D ** -0.5, 0.125, ((0, 4), (1, 8))),
        "rope_weight": gaussian(arg_keys[4], (D, QK_ROPE), D ** -0.5, 0.125),
        "query_up": gaussian(arg_keys[5], (Q_LAT, HEADS * QK_DIM), Q_LAT ** -0.5, 0.21875, ((0, 4), (1, 8))),
        "key_up": gaussian(arg_keys[6], (KV_LAT, HEADS * QK_NOPE), KV_LAT ** -0.5, 0.25, ((0, 4), (1, 8))),
        "value_up": gaussian(arg_keys[7], (KV_LAT, HEADS * V_DIM), KV_LAT ** -0.5, 0.25, ((0, 4), (1, 8))),
        "latent_gain": jnp.clip(1.0 + 0.18 * jax.random.normal(arg_keys[8], (Q_LAT,), jnp.float32), 0.1, 1.9),
        "memory_gain": jnp.clip(1.0 + 0.18 * jax.random.normal(arg_keys[9], (KV_LAT,), jnp.float32), 0.1, 1.9),
        "query_gain": draw_query_gain(jax.random.fold_in(arg_keys[19], 71), 0),
        "key_gain": jnp.clip(1.0 + 0.18 * jax.random.normal(arg_keys[11], (QK_DIM,), jnp.float32), 0.1, 1.9),
        "conv_value": draw_conv_value(jax.random.fold_in(arg_keys[19], 71), 0),
        "conv_gate": gaussian(arg_keys[13], (D, CONV_W), D ** -0.5, 0.125, ((0, 4), (1, 8))),
        "conv_kernel": draw_conv_kernel(jax.random.fold_in(arg_keys[19], 71), 0),
        "channel_gain": jnp.clip(1.0 + 0.18 * jax.random.normal(arg_keys[15], (CONV_W,), jnp.float32), 0.1, 1.9),
        "channel_shift": gaussian(arg_keys[16], (CONV_W,), 0.5, 3.0, ((0, 8),), jnp.float32),
        "heads_out": gaussian(arg_keys[17], (HEADS * V_DIM, D), V_DIM ** -0.5, 0.75, ((0, 8), (1, 4))),
        "conv_out": gaussian(arg_keys[18], (CONV_W, D), CONV_W ** -0.5, 0.1875, ((0, 8), (1, 4))),
    }


epsilon = 1e-06
rope_base = 10000.0
masked_score = -1e+30

def norm_rows(matrix, scale_vector):
    return matrix * lax.rsqrt(lax.optimization_barrier(jnp.mean(matrix * matrix, axis=-1, keepdims=True)) + epsilon) * scale_vector.astype(jnp.float32)

def rope_tables(positions):
    inverse_freq = 1.0 / rope_base ** (jnp.arange(0, QK_ROPE, 2, dtype=jnp.float32) / QK_ROPE)
    angles = positions.astype(jnp.float32)[:, None] * inverse_freq[None, :]
    return (jnp.cos(angles)[:, None, :], jnp.sin(angles)[:, None, :])

def rotate(matrix, cosine_table, sine_table):
    half_width = matrix.shape[-1] // 2
    front_half = matrix[..., :half_width]
    back_half = matrix[..., half_width:]
    return jnp.concatenate([front_half * cosine_table - back_half * sine_table, front_half * sine_table + back_half * cosine_table], axis=-1)

def heads_query(latent, weight, scale_vector, cosine_table, sine_table):
    row_count = latent.shape[0]
    projected = jnp.dot(latent, weight, preferred_element_type=jnp.float32)
    projected = norm_rows(projected.reshape(row_count, weight.shape[1] // QK_DIM, QK_DIM), scale_vector)
    turned = rotate(projected[..., QK_NOPE:], cosine_table, sine_table)
    return jnp.concatenate([projected[..., :QK_NOPE], turned], axis=-1).astype(jnp.bfloat16)

def heads_key(latent, rope_rows, weight, scale_vector, cosine_table, sine_table):
    row_count = latent.shape[0]
    head_count = weight.shape[1] // QK_NOPE
    nope_part = jnp.dot(latent, weight, preferred_element_type=jnp.float32).reshape(row_count, head_count, QK_NOPE)
    shared = jnp.broadcast_to(rope_rows.astype(jnp.float32)[:, None, :], (row_count, head_count, QK_ROPE))
    joined = norm_rows(jnp.concatenate([nope_part, shared], axis=-1), scale_vector)
    turned = rotate(joined[..., QK_NOPE:], cosine_table, sine_table)
    return jnp.concatenate([joined[..., :QK_NOPE], turned], axis=-1).astype(jnp.bfloat16)

def depthwise(extended, kernel, row_count):

    def add_tap(tap_index, running):
        window = lax.dynamic_slice_in_dim(extended, tap_index.astype(jnp.int32), row_count, 0).astype(jnp.float32)
        weight_row = lax.dynamic_slice_in_dim(kernel, tap_index.astype(jnp.int32), 1, 0).astype(jnp.float32)
        return running + window * weight_row
    return lax.fori_loop(0, kernel.shape[0], add_tap, jnp.zeros((row_count, kernel.shape[1]), jnp.float32))

def attention_block(queries, key_rows, value_rows, query_pos):
    key_pos = jnp.arange(key_rows.shape[0], dtype=jnp.int32)
    scores = jnp.einsum('qhd,khd->qhk', queries.astype(jnp.float32), key_rows.astype(jnp.float32)) * QK_DIM ** (-0.5)
    allowed = ((key_pos // SEG)[None, :] <= (query_pos // SEG)[:, None])[:, None, :]
    scores = jnp.where(allowed, scores, masked_score)
    row_max = lax.optimization_barrier(jnp.max(scores, axis=2, keepdims=True))
    weights = jnp.where(allowed, jnp.exp(scores - row_max), 0.0)
    row_total = lax.optimization_barrier(jnp.sum(weights, axis=2))
    rounded = weights.astype(jnp.bfloat16)
    summed = jnp.einsum('qhk,khd->qhd', rounded.astype(jnp.float32), value_rows.astype(jnp.float32))
    return (summed / row_total[:, :, None]).astype(jnp.bfloat16)

def one_sequence(tokens, mix_gain, query_down, memory_down, rope_weight, query_up, key_up, value_up, latent_gain, memory_gain, query_gain, key_gain, conv_value, conv_gate, conv_kernel, channel_gain, channel_shift, heads_out, conv_out):
    normed = norm_rows(tokens.astype(jnp.float32), mix_gain).astype(jnp.bfloat16)
    latent_query = jnp.dot(normed, query_down, preferred_element_type=jnp.float32).astype(jnp.bfloat16)
    latent_memory = jnp.dot(normed, memory_down, preferred_element_type=jnp.float32).astype(jnp.bfloat16)
    rope_rows = jnp.dot(normed, rope_weight, preferred_element_type=jnp.float32).astype(jnp.bfloat16)
    value_part = jnp.dot(normed, conv_value, preferred_element_type=jnp.float32)
    gate_part = jnp.dot(normed, conv_gate, preferred_element_type=jnp.float32)
    gated = (value_part * jax.nn.sigmoid(gate_part)).astype(jnp.bfloat16)
    query_normed = norm_rows(latent_query.astype(jnp.float32), latent_gain).astype(jnp.bfloat16)
    memory_normed = norm_rows(latent_memory.astype(jnp.float32), memory_gain).astype(jnp.bfloat16)
    positions = jnp.arange(SEQ, dtype=jnp.int32)
    cosine_table, sine_table = rope_tables(positions)
    queries = heads_query(query_normed, query_up, query_gain, cosine_table, sine_table)
    key_rows = heads_key(memory_normed, rope_rows, key_up, key_gain, cosine_table, sine_table)
    value_rows = jnp.dot(memory_normed, value_up, preferred_element_type=jnp.float32).astype(jnp.bfloat16).reshape(SEQ, HEADS, V_DIM)
    query_blocks = queries.reshape(SEQ // TOK_DEV, TOK_DEV, HEADS, QK_DIM)
    block_pos = positions.reshape(SEQ // TOK_DEV, TOK_DEV)

    def per_block(pair):
        return attention_block(pair[0], key_rows, value_rows, pair[1])
    attention = lax.map(per_block, (query_blocks, block_pos)).reshape(SEQ, HEADS * V_DIM)
    extended = jnp.concatenate([jnp.zeros((CONV_K - 1, CONV_W), jnp.bfloat16), gated], axis=0)
    conv_sum = depthwise(extended, conv_kernel, SEQ)
    row_mean = lax.optimization_barrier(jnp.mean(conv_sum, axis=1, keepdims=True))
    centered = conv_sum - row_mean
    spread = lax.optimization_barrier(jnp.mean(centered * centered, axis=1, keepdims=True))
    conv_result = jax.nn.silu(centered * lax.rsqrt(spread + epsilon) * channel_gain.astype(jnp.float32) + channel_shift.astype(jnp.float32)).astype(jnp.bfloat16)
    attn_width = HEADS * V_DIM // N_TP
    conv_width = CONV_W // N_TP
    mixed = jnp.zeros((SEQ, D), jnp.float32)
    for group_index in range(N_TP):
        head_cols = slice(group_index * attn_width, (group_index + 1) * attn_width)
        conv_cols = slice(group_index * conv_width, (group_index + 1) * conv_width)
        partial_sum = jnp.dot(attention[:, head_cols], heads_out[head_cols], preferred_element_type=jnp.float32)
        partial_sum = partial_sum + jnp.dot(conv_result[:, conv_cols], conv_out[conv_cols], preferred_element_type=jnp.float32)
        mixed = mixed + lax.optimization_barrier(partial_sum.astype(jnp.bfloat16)).astype(jnp.float32)
    return mixed.astype(jnp.bfloat16)

def reference(tokens, mix_gain, query_down, memory_down, rope_weight, query_up, key_up, value_up, latent_gain, memory_gain, query_gain, key_gain, conv_value, conv_gate, conv_kernel, channel_gain, channel_shift, heads_out, conv_out):

    def per_sequence(sequence):
        return one_sequence(sequence, mix_gain, query_down, memory_down, rope_weight, query_up, key_up, value_up, latent_gain, memory_gain, query_gain, key_gain, conv_value, conv_gate, conv_kernel, channel_gain, channel_shift, heads_out, conv_out)
    return lax.map(per_sequence, tokens)
```

```python
import functools
import math

import jax
import jax.numpy as jnp
from jax import lax
from jax.experimental import pallas as pl
from jax.experimental.pallas import tpu as pltpu
from jax.sharding import PartitionSpec as P

D = 2048
ROWS = 256
QK_NOPE = 64
QK_ROPE = 32
QK_DIM = 96
V_DIM = 64
Q_LAT = 768
KV_LAT = 512
CONV_W = 1024
CONV_K = 31
SEG = 64
N_SP = 16
N_FS = 4
N_TP = 8
HEAD_ROWS = QK_DIM + V_DIM

epsilon = 1e-06
rope_base = 10000.0
masked_score = -1e30
score_scale = QK_DIM**-0.5 * math.log2(math.e)

F32 = jnp.float32
BF16 = jnp.bfloat16


def remote(src, dst, send, recv, **where):
    return pltpu.make_async_remote_copy(
        src_ref=src,
        dst_ref=dst,
        send_sem=send,
        recv_sem=recv,
        device_id=where,
        device_id_type=pl.DeviceIdType.MESH,
    )


def dot(a, b, contract=(1, 0)):
    return lax.dot_general(
        a, b, (((contract[0],), (contract[1],)), ((), ())), preferred_element_type=F32
    )


def column(row, width):
    n = row.shape[1]
    tall = jnp.broadcast_to(row, (128, n)).T
    return jnp.concatenate([tall] * (width // 128), axis=1)


def turned(block, cosine, sine):
    a, b = block[:16], block[16:]
    return jnp.concatenate([a * cosine - b * sine, a * sine + b * cosine], axis=0)


def kernel(
    tokens_h, md_h, qd_h, qu_h, ku_h, vu_h, cv_h, cg_h, ho_h, co_h,
    mix_gain, rope_weight, latent_gain, memory_gain, query_gain, key_gain,
    conv_kernel, channel_gain, channel_shift, tables,
    out_h,
    tok, nrm, MD, KVU, QD, QU, CV, HC, LM, LQ, KV, qt, stat, halo, ext, cmix,
    sm_max, sm_sum, sm_acc, part, pair_in, total, r1, s2, r2, outv,
    load_sem, ys, yr, ts, tr, zs, zr, hs, hr, ds, dr, xs, xr, out_sem,
):
    z = lax.axis_index("sp")
    f = lax.axis_index("fs")
    t = lax.axis_index("tp")
    x = t // 2
    core = t % 2

    loads = []

    def load(src, dst):
        copy = pltpu.make_async_copy(src, dst, load_sem.at[len(loads)])
        copy.start()
        loads.append(copy)
        return len(loads) - 1

    load(md_h, MD.at[f])
    load(tokens_h.at[0], tok)
    load(ku_h, KVU.at[f, :, pl.ds(0, 128)])
    load(vu_h, KVU.at[f, :, pl.ds(128, 128)])
    load(qd_h, QD.at[f])
    load(qu_h, QU.at[f])
    load(cv_h, CV.at[f, :, pl.ds(0, 128)])
    load(cg_h, CV.at[f, :, pl.ds(128, 128)])
    load(ho_h, HC.at[f, pl.ds(0, 128)])
    load(co_h, HC.at[f, pl.ds(128, 128)])

    barrier = pltpu.get_barrier_semaphore()
    for d in range(1, N_FS):
        pl.semaphore_signal(
            barrier, inc=1, device_id={"fs": (f + d) % N_FS}, device_id_type=pl.DeviceIdType.MESH
        )
    for d in range(1, N_TP):
        pl.semaphore_signal(
            barrier, inc=1, device_id={"tp": (t + d) % N_TP}, device_id_type=pl.DeviceIdType.MESH
        )
    for d in (1, N_SP - 1):
        pl.semaphore_signal(
            barrier, inc=1, device_id={"sp": (z + d) % N_SP}, device_id_type=pl.DeviceIdType.MESH
        )
    pl.semaphore_wait(barrier, N_FS - 1 + N_TP - 1 + 2)

    up, down = (f + 1) % N_FS, (f + N_FS - 1) % N_FS
    far = (f + 2) % N_FS
    weights = [MD, KVU, QD, QU, CV, HC]

    def y_copies(i):
        buf = weights[i]
        half = buf.shape[1] // 2
        top, low = pl.ds(0, half), pl.ds(half, half)
        own_up = remote(buf.at[f], buf.at[f], ys.at[i, 0], yr.at[i, 0], fs=up)
        own_down = remote(buf.at[f], buf.at[f], ys.at[i, 1], yr.at[i, 1], fs=down)
        fwd_up = remote(buf.at[down, top], buf.at[down, top], ys.at[i, 2], yr.at[i, 2], fs=up)
        fwd_down = remote(buf.at[up, low], buf.at[up, low], ys.at[i, 3], yr.at[i, 3], fs=down)
        in_down = remote(buf.at[down], buf.at[down], ys.at[i, 0], yr.at[i, 0], fs=up)
        in_up = remote(buf.at[up], buf.at[up], ys.at[i, 1], yr.at[i, 1], fs=down)
        in_far_top = remote(buf.at[far, top], buf.at[far, top], ys.at[i, 2], yr.at[i, 2], fs=up)
        in_far_low = remote(buf.at[far, low], buf.at[far, low], ys.at[i, 3], yr.at[i, 3], fs=down)
        return own_up, own_down, fwd_up, fwd_down, in_down, in_up, in_far_top, in_far_low

    def y_send(i):
        c = y_copies(i)
        c[0].start()
        c[1].start()

    def y_forward(i):
        c = y_copies(i)
        c[4].wait_recv()
        c[2].start()
        c[5].wait_recv()
        c[3].start()

    def y_finish(i):
        c = y_copies(i)
        c[6].wait_recv()
        c[7].wait_recv()

    def tp_send(k, buf):
        def body(d, _):
            remote(buf.at[t], buf.at[t], ts.at[k, d], tr.at[k, d], tp=(t + d) % N_TP).start()
            return 0

        lax.fori_loop(1, N_TP, body, 0)

    def tp_wait(k, buf):
        def body(d, _):
            src = (t + N_TP - d) % N_TP
            remote(buf.at[src], buf.at[src], ts.at[k, d], tr.at[k, d], tp=src).wait_recv()
            return 0

        lax.fori_loop(1, N_TP, body, 0)

    ahead, behind = (z + 1) % N_SP, (z + N_SP - 1) % N_SP

    def z_copy(way, step, h, slot):
        piece = KV.at[slot, pl.ds(h * HEAD_ROWS, HEAD_ROWS)]
        return remote(
            piece, piece, zs.at[way, step, h], zr.at[way, step, h], sp=ahead if way == 0 else behind
        )

    def attend(slot, own):
        def one_head(h, _):
            keys = KV[slot, pl.ds(h * HEAD_ROWS, QK_DIM), :]
            vals = KV[slot, pl.ds(h * HEAD_ROWS + QK_DIM, V_DIM), :]
            s = dot(keys, qt[h], (0, 0)) * score_scale
            if own:
                k_seg = lax.broadcasted_iota(jnp.int32, (ROWS, ROWS), 0) // SEG
                q_seg = lax.broadcasted_iota(jnp.int32, (ROWS, ROWS), 1) // SEG
                s = jnp.where(k_seg <= q_seg, s, masked_score)
                new_max = jnp.max(s, axis=0, keepdims=True)
                w = jnp.exp2(s - new_max)
                sm_sum[h] = jnp.sum(w, axis=0, keepdims=True)
                sm_acc[h] = dot(vals, w.astype(BF16))
            else:
                old = sm_max[h]
                new_max = jnp.maximum(old, jnp.max(s, axis=0, keepdims=True))
                w = jnp.exp2(s - new_max)
                factor = jnp.exp2(old - new_max)
                sm_sum[h] = sm_sum[h] * factor + jnp.sum(w, axis=0, keepdims=True)
                sm_acc[h] = sm_acc[h] * factor + dot(vals, w.astype(BF16))
            sm_max[h] = new_max
            return 0

        lax.fori_loop(0, 2, one_head, 0)

    def z_step(step, both):
        slot_a = (z + N_SP - step) % N_SP
        slot_b = (z + step) % N_SP
        for h in range(2):
            z_copy(0, step - 1, h, slot_a).wait_recv()
            if both:
                z_copy(0, step, h, slot_a).start()
                z_copy(1, step - 1, h, slot_b).wait_recv()

                @pl.when(step < N_SP // 2 - 1)
                def _():
                    z_copy(1, step, h, slot_b).start()

    def z_attend(step, both):
        slot_a = (z + N_SP - step) % N_SP
        slot_b = (z + step) % N_SP

        @pl.when(z >= step)
        def _():
            attend(slot_a, False)

        if both:

            @pl.when(z + step >= N_SP)
            def _():
                attend(slot_b, False)

    def after_load(*which):
        for i in which:
            loads[i].wait()

    after_load(0)
    y_send(0)
    after_load(2, 3)
    y_send(1)

    after_load(1)
    own = tok[...].astype(F32)
    inv = lax.rsqrt(jnp.mean(own * own, axis=1, keepdims=True) + epsilon)
    nrm[...] = (own * inv * mix_gain[...]).astype(BF16)

    y_forward(0)
    after_load(4)
    y_send(2)
    rope_rows = dot(nrm[...], rope_weight[...])
    rope_t = jnp.concatenate([rope_rows, jnp.zeros((ROWS, 96), F32)], axis=1).T[:QK_ROPE]
    rope_t = rope_t.astype(BF16).astype(F32)
    y_finish(0)
    acc = jnp.zeros((ROWS, 128), F32)
    for g in range(N_FS):
        w = MD[g]
        left = dot(nrm[:, g * 512 : g * 512 + 256], w)
        right = dot(nrm[:, g * 512 + 256 : g * 512 + 512], w)
        acc = acc + jnp.concatenate([left[:, :64], right[:, 64:]], axis=1)
    acc_t = acc.T
    LM[t] = (acc_t[:64] + acc_t[64:]).astype(BF16)
    tp_send(0, LM)

    y_forward(1)
    after_load(5)
    y_send(3)

    cosine, sine = tables[:16], tables[16:]
    y_finish(1)
    tp_wait(0, LM)
    mem = LM[...].reshape(KV_LAT, ROWS).astype(F32)
    mem_inv = lax.rsqrt(jnp.mean(mem * mem, axis=0, keepdims=True) + epsilon)
    mem_n = (mem * mem_inv * column(memory_gain[...], ROWS)).astype(BF16)
    both_up = dot(KVU[...].reshape(KV_LAT, 256), mem_n, (0, 0))
    k_gain = column(key_gain[...], ROWS)
    rope_sq = jnp.sum(rope_t * rope_t, axis=0, keepdims=True)
    rope_g = turned(rope_t * k_gain[QK_NOPE:QK_DIM], cosine, sine)
    for h in range(2):
        nope = both_up[h * 64 : h * 64 + 64]
        mean = (jnp.sum(nope * nope, axis=0, keepdims=True) + rope_sq) * (1.0 / QK_DIM)
        k_inv = lax.rsqrt(mean + epsilon)
        KV[z, h * HEAD_ROWS : h * HEAD_ROWS + QK_NOPE] = (nope * k_inv * k_gain[:QK_NOPE]).astype(BF16)
        KV[z, h * HEAD_ROWS + QK_NOPE : h * HEAD_ROWS + QK_DIM] = (rope_g * k_inv).astype(BF16)
        KV[z, h * HEAD_ROWS + QK_DIM : (h + 1) * HEAD_ROWS] = both_up[
            128 + h * 64 : 192 + h * 64
        ].astype(BF16)
    for h in range(2):
        z_copy(0, 0, h, z).start()
        z_copy(1, 0, h, z).start()

    y_forward(2)
    after_load(6, 7)
    y_send(4)
    y_finish(2)
    acc = jnp.zeros((ROWS, 96), F32)
    for g in range(N_FS):
        acc = acc + dot(nrm[:, g * 512 : g * 512 + 512], QD[g])
    acc_t = jnp.concatenate([acc, jnp.zeros((ROWS, 32), F32)], axis=1).T
    LQ[t] = acc_t[:96].astype(BF16)
    tp_send(1, LQ)
    y_forward(3)
    after_load(8, 9)

    z_step(1, True)
    y_finish(3)
    tp_wait(1, LQ)
    lat = LQ[...].reshape(Q_LAT, ROWS).astype(F32)
    lat_inv = lax.rsqrt(jnp.mean(lat * lat, axis=0, keepdims=True) + epsilon)
    lat_n = (lat * lat_inv * column(latent_gain[...], ROWS)).astype(BF16)
    q_all = dot(QU[...].reshape(Q_LAT, 192), lat_n, (0, 0))
    q_gain = column(query_gain[...], ROWS)
    for h in range(2):
        q = q_all[h * QK_DIM : (h + 1) * QK_DIM]
        q = q * lax.rsqrt(jnp.mean(q * q, axis=0, keepdims=True) + epsilon) * q_gain[:QK_DIM]
        qt[h, :QK_NOPE] = q[:QK_NOPE].astype(BF16)
        qt[h, QK_NOPE:] = turned(q[QK_NOPE:], cosine, sine).astype(BF16)
    attend(z, True)
    z_attend(1, True)

    z_step(2, True)
    y_forward(4)
    y_send(5)
    z_attend(2, True)

    z_step(3, True)
    z_attend(3, True)
    y_finish(4)
    gates = jnp.zeros((ROWS, 256), F32)
    for g in range(N_FS):
        gates = gates + dot(nrm[:, g * 512 : g * 512 + 512], CV[g])
    gated = (gates[:, :128] * jax.nn.sigmoid(gates[:, 128:])).astype(BF16)
    ext[32:, :] = gated.astype(F32)
    halo[0] = gated[ROWS - 32 :]
    halo_copy = remote(halo.at[0], halo.at[1], hs, hr, sp=ahead)
    halo_copy.start()

    z_step(4, True)
    y_forward(5)
    z_attend(4, True)

    halo_copy.wait_recv()
    ext[:32, :] = jnp.where(z > 0, halo[1].astype(F32), 0.0)
    taps = conv_kernel[...].astype(F32)
    sums = jnp.zeros((ROWS, 128), F32)
    for j in range(CONV_K):
        sums = sums + ext[2 + j : 2 + j + ROWS, :] * taps[j : j + 1]
    conv = sums.T
    own_mean = jnp.mean(conv, axis=0, keepdims=True)
    off = conv - own_mean
    own_m2 = jnp.sum(off * off, axis=0, keepdims=True)
    stat[t] = jnp.concatenate([own_mean, own_m2, jnp.zeros((6, ROWS), F32)], axis=0)
    cmix[...] = conv
    tp_send(2, stat)

    z_step(5, True)
    z_attend(5, True)

    tp_wait(2, stat)
    means = stat[:, 0, :]
    m2 = stat[:, 1, :]
    row_mean = jnp.mean(means, axis=0, keepdims=True)
    drift = means - row_mean
    spread = jnp.sum(m2 + 128.0 * drift * drift, axis=0, keepdims=True) * (1.0 / CONV_W)
    v = (cmix[...] - row_mean) * lax.rsqrt(spread + epsilon)
    v = v * column(channel_gain[...], ROWS) + column(channel_shift[...], ROWS)
    cmix[...] = v / (1.0 + jnp.exp(-v))

    z_step(6, True)
    y_finish(5)
    z_attend(6, True)
    z_step(7, True)
    z_attend(7, True)
    z_step(8, False)
    z_attend(8, False)

    mixed = [(sm_acc[h] / sm_sum[h]) for h in range(2)]
    mix_rows = jnp.concatenate(mixed + [cmix[...]], axis=0).T.astype(BF16)
    for g in range(N_FS):
        block = dot(mix_rows, HC[g]).astype(BF16)
        part[:, :, :, g * 512 : g * 512 + 512] = block.reshape(2, 4, 32, 512)
    partner = t + 1 - 2 * core
    pair_copy = remote(part.at[1 - core], pair_in, ds.at[0], dr.at[0], tp=partner)
    pair_copy.start()
    pair_copy.wait_recv()

    near = x + 1 - 2 * (x % 2)
    across = 3 - x
    cols = (pl.ds(0, 1024), pl.ds(1024, 1024))
    first = (near, across)
    second = (across, near)

    def other(g, s):
        return g + 1 - 2 * (g % 2) if s == 0 else 3 - g

    total[...] = (part[core].astype(F32) + pair_in[...].astype(F32)).astype(BF16)

    def halve1(s, k):
        g = first[s] if k == 0 else other(first[s], 1 - s)
        return remote(
            total.at[g, :, cols[s]], r1.at[s, k], xs.at[0, s, k], xr.at[0, s, k], tp=2 * first[s] + core
        )

    for k in (1, 0):
        for s in range(2):
            halve1(s, k).start()
    for s in range(2):
        halve1(s, 1).wait_recv()
        g = second[s]
        s2[s] = (total[g, :, s * 1024 : (s + 1) * 1024].astype(F32) + r1[s, 1].astype(F32)).astype(BF16)

        def halve2(s=s):
            return remote(s2.at[s], r2.at[s], xs.at[1, s, 0], xr.at[1, s, 0], tp=2 * second[s] + core)

        halve2().start()

    def out_piece(c, g, s):
        return outv.at[c, g, :, cols[s]]

    def gather1(s, g):
        p = out_piece(core, g, s)
        return remote(p, p, xs.at[2, s, 0], xr.at[2, s, 0], tp=2 * second[s] + core)

    def gather2(s, k, g):
        p = out_piece(core, g, s)
        return remote(p, p, xs.at[3, s, k], xr.at[3, s, k], tp=2 * first[s] + core)

    def to_pair(s, k, c, g):
        p = out_piece(c, g, s)
        return remote(p, p, ds.at[1 + s * 4 + k], dr.at[1 + s * 4 + k], tp=partner)

    for s in range(2):
        halve1(s, 0).wait_recv()
        remote(
            s2.at[s], r2.at[s], xs.at[1, s, 0], xr.at[1, s, 0], tp=2 * second[s] + core
        ).wait_recv()
        mine = (
            total[x, :, s * 1024 : (s + 1) * 1024].astype(F32)
            + r1[s, 0].astype(F32)
            + r2[s].astype(F32)
        )
        outv[core, x, :, s * 1024 : (s + 1) * 1024] = mine.astype(BF16)
        gather1(s, x).start()
        gather2(s, 0, x).start()
        to_pair(s, 0, core, x).start()
    for s in range(2):
        gather1(s, second[s]).wait_recv()
        gather2(s, 1, second[s]).start()
        to_pair(s, 1, core, second[s]).start()
    for s in range(2):
        g0, g1 = first[s], other(first[s], 1 - s)
        gather2(s, 0, g0).wait_recv()
        to_pair(s, 2, core, g0).start()
        gather2(s, 1, g1).wait_recv()
        to_pair(s, 3, core, g1).start()
    for s in range(2):
        groups = (x, second[s], first[s], other(first[s], 1 - s))
        for k in range(4):
            to_pair(s, k, 1 - core, groups[k]).wait_recv()
    copies = []
    for c in range(2):
        for g in range(4):
            copy = pltpu.make_async_copy(
                outv.at[c, g], out_h.at[0, pl.ds(c * 128 + g * 32, 32)], out_sem.at[c, g]
            )
            copy.start()
            copies.append(copy)
    for copy in copies:
        copy.wait()

    for i in range(len(weights)):
        for copy in y_copies(i)[:4]:
            copy.wait_send()
    for k, buf in ((0, LM), (1, LQ), (2, stat)):

        def sent(d, _, k=k, buf=buf):
            remote(buf.at[t], buf.at[t], ts.at[k, d], tr.at[k, d], tp=(t + d) % N_TP).wait_send()
            return 0

        lax.fori_loop(1, N_TP, sent, 0)

    def z_sent(step, _):
        for h in range(2):
            z_copy(0, step, h, (z + N_SP - step) % N_SP).wait_send()

            @pl.when(step < N_SP // 2 - 1)
            def _():
                z_copy(1, step, h, (z + step) % N_SP).wait_send()

        return 0

    lax.fori_loop(0, N_SP // 2, z_sent, 0)
    halo_copy.wait_send()
    pair_copy.wait_send()
    for s in range(2):
        for k in range(2):
            halve1(s, k).wait_send()
        remote(s2.at[s], r2.at[s], xs.at[1, s, 0], xr.at[1, s, 0], tp=2 * second[s] + core).wait_send()
        gather1(s, x).wait_send()
        gather2(s, 0, x).wait_send()
        gather2(s, 1, second[s]).wait_send()
        groups = (x, second[s], first[s], other(first[s], 1 - s))
        for k in range(4):
            to_pair(s, k, core, groups[k]).wait_send()


def local(
    tokens, mix_gain, query_down, memory_down, rope_weight, query_up, key_up, value_up,
    latent_gain, memory_gain, query_gain, key_gain, conv_value, conv_gate, conv_kernel,
    channel_gain, channel_shift, heads_out, conv_out,
):
    memory_pairs = jnp.concatenate([memory_down[:256], memory_down[256:]], axis=1)
    positions = (lax.axis_index("sp") * ROWS + jnp.arange(ROWS, dtype=jnp.int32)).astype(F32)
    inverse_freq = 1.0 / rope_base ** (jnp.arange(0, QK_ROPE, 2, dtype=F32) / QK_ROPE)
    angles = inverse_freq[:, None] * positions[None, :]
    tables = jnp.concatenate([jnp.cos(angles), jnp.sin(angles)], axis=0)

    def row(v):
        v = v.reshape(1, -1)
        return jnp.pad(v, ((0, 0), (0, -v.shape[1] % 128)))

    hbm = pl.BlockSpec(memory_space=pl.ANY)
    vmem = pl.BlockSpec(memory_space=pltpu.VMEM)
    dma = pltpu.SemaphoreType.DMA
    return pl.pallas_call(
        kernel,
        out_shape=jax.ShapeDtypeStruct((1, ROWS, D), BF16),
        in_specs=[hbm] * 10 + [vmem] * 10,
        out_specs=hbm,
        scratch_shapes=[
            pltpu.VMEM((ROWS, D), BF16),
            pltpu.VMEM((ROWS, D), BF16),
            pltpu.VMEM((N_FS, 256, 128), BF16),
            pltpu.VMEM((N_FS, 128, 256), BF16),
            pltpu.VMEM((N_FS, 512, 96), BF16),
            pltpu.VMEM((N_FS, 192, 192), BF16),
            pltpu.VMEM((N_FS, 512, 256), BF16),
            pltpu.VMEM((N_FS, 256, 512), BF16),
            pltpu.VMEM((N_TP, 64, ROWS), BF16),
            pltpu.VMEM((N_TP, 96, ROWS), BF16),
            pltpu.VMEM((N_SP, 2 * HEAD_ROWS, ROWS), BF16),
            pltpu.VMEM((2, QK_DIM, ROWS), BF16),
            pltpu.VMEM((N_TP, 8, ROWS), F32),
            pltpu.VMEM((2, 32, 128), BF16),
            pltpu.VMEM((ROWS + 32, 128), F32),
            pltpu.VMEM((128, ROWS), F32),
            pltpu.VMEM((2, 1, ROWS), F32),
            pltpu.VMEM((2, 1, ROWS), F32),
            pltpu.VMEM((2, V_DIM, ROWS), F32),
            pltpu.VMEM((2, 4, 32, D), BF16),
            pltpu.VMEM((4, 32, D), BF16),
            pltpu.VMEM((4, 32, D), BF16),
            pltpu.VMEM((2, 2, 32, 1024), BF16),
            pltpu.VMEM((2, 32, 1024), BF16),
            pltpu.VMEM((2, 32, 1024), BF16),
            pltpu.VMEM((2, 4, 32, D), BF16),
            dma((10,)),
            dma((6, 4)),
            dma((6, 4)),
            dma((3, N_TP)),
            dma((3, N_TP)),
            dma((2, N_SP // 2, 2)),
            dma((2, N_SP // 2, 2)),
            dma,
            dma,
            dma((9,)),
            dma((9,)),
            dma((4, 2, 2)),
            dma((4, 2, 2)),
            dma((2, 4)),
        ],
        compiler_params=pltpu.CompilerParams(
            collective_id=0, has_side_effects=True, vmem_limit_bytes=40 * 1024 * 1024
        ),
        name="layer",
    )(
        tokens, memory_pairs, query_down, query_up, key_up, value_up, conv_value, conv_gate,
        heads_out, conv_out,
        row(mix_gain), rope_weight, row(latent_gain), row(memory_gain), row(query_gain),
        row(key_gain), conv_kernel, row(channel_gain), row(channel_shift), tables,
    )


def solution(mesh):
    in_specs = (
        P("fs", "sp", None),
        P(),
        P("fs", "tp"),
        P("fs", "tp"),
        P(),
        P("fs", "tp"),
        P("fs", "tp"),
        P("fs", "tp"),
        P(),
        P(),
        P(),
        P(),
        P("fs", "tp"),
        P("fs", "tp"),
        P(None, "tp"),
        P("tp"),
        P("tp"),
        P("tp", "fs"),
        P("tp", "fs"),
    )
    out_specs = P("fs", "sp", None)
    return jax.shard_map(local, mesh=mesh, in_specs=in_specs, out_specs=out_specs, check_vma=False)
```
